32 devices in a mesh: ep: 8 (over z, core), tp: 4 (over y, x).
Axes of the slice: x: 2, y: 2, z: 4, core: 2. Of those that a mesh axis runs over, the one named last changes fastest.
Arguments:
- mixer_rows: bfloat16 [4096, 2048], P('ep', 'tp'), may hold values from -6 to 6
- expert_rows: bfloat16 [4096, 2048], P('ep', 'tp'), may hold values from -6 to 6
- mixer_gain: float32 [2048], replicated, may hold values from 0.1 to 1.9
- pool_scale: float32 [2048], P('tp'), may hold values from 0.1 to 1.9
- w_in: bfloat16 [2048, 2048], P(None, 'tp'), may hold values from -0.125 to 0.125
- w_mix_out: bfloat16 [2048, 2048], P(None, 'tp'), may hold values from -0.125 to 0.125
- expert_gain: float32 [2048], replicated, may hold values from 0.1 to 1.9
- expert_gate: bfloat16 [8, 2048, 2048], P('ep', None, 'tp'), may hold values from -0.125 to 0.125
- expert_up: bfloat16 [8, 2048, 2048], P('ep', None, 'tp'), may hold values from -0.125 to 0.125
- expert_down: bfloat16 [8, 2048, 2048], P('ep', None, 'tp'), may hold values from -0.125 to 0.125
- routes: int32 [4096, 2], P('ep'), may hold values from 0 to 7, all different within a row; in each aligned block of 512 rows (0 to 511, 512 to 1023, ...) at most 192 rows name the same one
- route_weight: float32 [4096, 2], P('ep'), may hold values from 0.1 to 1
Outputs:
- mixer_output: bfloat16 [4096, 2048], P('ep', 'tp')
- expert_output: bfloat16 [4096, 2048], P('ep', 'tp')
The draws below stay inside these ranges and needn't reach their ends.
Inputs may be any that keep to these rules, and one draw needn't show every extreme that they name: `routes`: each row names 2 different experts. Among the rows of one device (aligned blocks of 512 rows) no expert is named more than 192 times, a bound that some block reaches.
All inputs are finite; a program needn't handle non-finite values.
Results may differ from the reference program's by a relative error of at most 0.0071.
Values may be sent and summed in bfloat16 or wider, within the bound.
No kernel may reach another device: no remote copies, remote signals or barrier semaphores. Data moves between devices by JAX's collectives and lax.ppermute only.
A program may use at most 64 MiB of HBM per device.

```python
import math
import jax
import jax.numpy as jnp
import numpy as np
from jax import lax

D = 2048
PW = 2048
FE = 2048
TOP = 2
TOK_DEV = 512
TOKENS = 4096
EXPERTS = 8
CAP = 192
N_EP = 8


def steps_of(own_key, dims, pieces, smallest, top_value):
    def one(axis_at, parts):
        draws = jax.random.uniform(jax.random.fold_in(jax.random.fold_in(own_key, 6), axis_at), (parts,), jnp.float32, smallest / len(pieces), top_value / len(pieces))
        return jnp.repeat(jnp.exp(draws), dims[axis_at] // parts).reshape((-1,) + (1,) * (len(dims) - axis_at - 1))

    loudness = one(*pieces[0])
    for cut in pieces[1:]:
        loudness = loudness * one(*cut)
    return loudness


def shared_out(key, own, number, rows, amount, top, most, skew):
    sequence = jax.random.permutation(key, amount)
    crowded, common = portions_of(amount, rows * top, most, skew, True), portions_of(amount, rows * top, most, skew, False)
    places = jnp.arange(amount)

    def named(tallies, turn):
        used = int((tallies > 0).sum())
        fixed = max(1, used // 4)
        moved = fixed + (places - fixed + turn * (used - fixed)) % max(1, amount - fixed)
        return jnp.zeros((amount,), jnp.int32).at[sequence[jnp.where(places < fixed, places, moved)]].set(jnp.asarray(tallies, jnp.int32))

    tallies = jnp.where(number % 4 == 0, named(crowded, number // 4), named(common, number - number // 4 - 1))
    mixed = jax.random.permutation(jax.random.fold_in(own, 3), amount)
    donor, sink = mixed[0:amount // 2 * 2:2], mixed[1:amount // 2 * 2:2]
    room = jnp.minimum(tallies[donor] - 1, most - tallies[sink]) // 2
    room = jnp.where((donor == sequence[0]) | (sink == sequence[0]) | (tallies[sink] == 0), 0, jnp.maximum(room, 0))
    moved = jax.random.randint(jax.random.fold_in(own, 4), (amount // 2,), 0, 1 << 20) % (room + 1)
    tallies = tallies.at[donor].add(-moved).at[sink].add(moved)
    members = jnp.searchsorted(jnp.cumsum(tallies), jnp.arange(rows * top), side="right").astype(jnp.int32)
    listing = members.reshape(top, rows).T
    listing = listing[jax.random.permutation(jax.random.fold_in(own, 1), rows)]
    turn = jax.random.randint(jax.random.fold_in(own, 2), (rows, 1), 0, top)
    return jnp.take_along_axis(listing, (jnp.arange(top)[None, :] + turn) % top, axis=1)


def portions_of(count, total, reach, slope, full):
    loads = [(1 << 20) // math.isqrt(grade ** slope) + 1 for grade in range(1, count + 1)]
    largest = reach if full else min(reach, max(-(-total // count), total * loads[0] // sum(loads)))
    least = 1 if total - largest >= count - 1 else 0
    holding, rest = [largest] + [least] * (count - 1), total - largest - least * (count - 1)
    while rest > 0:
        movable = [i for i in range(1, count) if holding[i] < largest] or [i for i in range(1, count) if holding[i] < reach]
        pool, remaining = sum([loads[i] for i in movable]), rest
        for i in movable:
            extra = min(reach - holding[i], max(1, remaining * loads[i] // pool), rest)
            holding[i] = holding[i] + extra
            rest = rest - extra
    return np.array(holding)


def gaussian(stream_key, extent, deviation, most, shards=(), kind=jnp.bfloat16):
    entries = jax.random.normal(stream_key, extent, jnp.float32) * deviation
    if len(shards) > 0:
        entries = steps_of(stream_key, extent, shards, -0.22, 0.18) * entries
    return jnp.clip(entries, min=-most, max=most).astype(kind)


def setup_inputs(seed: int = 0) -> dict:
    key_list = jax.random.split(jax.random.key(seed), 13)
    mixer_rows = gaussian(key_list[0], (TOKENS, D), 1.0, 6.0, ((0, 8), (1, 4)))
    expert_rows = gaussian(key_list[1], (TOKENS, D), 1.0, 6.0, ((0, 8), (1, 4)))
    mixer_gain = jnp.clip(1.0 + 0.18 * jax.random.normal(key_list[2], (D,), jnp.float32), 0.1, 1.9)
    pool_scale = jnp.clip(1.0 + 0.18 * jax.random.normal(key_list[3], (PW,), jnp.float32), 0.1, 1.9)
    w_in = gaussian(key_list[4], (D, PW), D ** -0.5, 0.125, ((1, 4),))
    w_mix_out = gaussian(key_list[5], (PW, D), PW ** -0.5, 0.125, ((1, 4),))
    expert_gain = jnp.clip(1.0 + 0.18 * jax.random.normal(key_list[6], (D,), jnp.float32), 0.1, 1.9)
    expert_gate = gaussian(key_list[7], (EXPERTS, D, FE), D ** -0.5, 0.125, ((0, 8), (2, 4)))
    expert_up = gaussian(key_list[8], (EXPERTS, D, FE), D ** -0.5, 0.125, ((0, 8), (2, 4)))
    expert_down = gaussian(key_list[9], (EXPERTS, FE, D), FE ** -0.5, 0.125, ((0, 8), (2, 4)))
    routes_keys = jax.random.split(jax.random.fold_in(key_list[10], 1), TOKENS // TOK_DEV)
    routes_turns = jax.random.permutation(jax.random.fold_in(key_list[10], 3), TOKENS // TOK_DEV)
    routes = jax.vmap(lambda own, number: shared_out(jax.random.fold_in(key_list[10], 2), own, number, TOK_DEV, EXPERTS, TOP, CAP, 1))(routes_keys, routes_turns).reshape((TOKENS, TOP))
    route_weight = jnp.clip(jnp.exp(math.log(1.0) - 2.3025851 * jax.random.uniform(key_list[11], (TOKENS, TOP), jnp.float32) ** steps_of(key_list[11], (TOKENS, TOP), ((0, 8),), -0.2, 0.2)), 0.1, 1.0)
    return {"mixer_rows": mixer_rows, "expert_rows": expert_rows, "mixer_gain": mixer_gain, "pool_scale": pool_scale, "w_in": w_in, "w_mix_out": w_mix_out, "expert_gain": expert_gain, "expert_gate": expert_gate, "expert_up": expert_up, "expert_down": expert_down, "routes": routes, "route_weight": route_weight}


norm_eps = 1e-05
pool_windows = (2, 4, 8, 16)

def layer_norm(row_block, gain_vec):
    values = row_block.astype(jnp.float32)
    center = values - lax.optimization_barrier(jnp.mean(values, axis=-1, keepdims=True))
    spread = lax.optimization_barrier(jnp.mean(center * center, axis=-1, keepdims=True))
    return (center * lax.rsqrt(spread + norm_eps) * gain_vec).astype(jnp.bfloat16)

def reference(mixer_rows, expert_rows, mixer_gain, pool_scale, w_in, w_mix_out, expert_gain, expert_gate, expert_up, expert_down, routes, route_weight):
    normed_mix = layer_norm(mixer_rows, mixer_gain)
    inner_proj = jnp.dot(normed_mix, w_in, preferred_element_type=jnp.float32).astype(jnp.bfloat16)
    values = inner_proj.astype(jnp.float32)
    seq_len = values.shape[0]
    prefix = jnp.concatenate([jnp.zeros((1, PW), jnp.float32), jnp.cumsum(values, axis=0)], axis=0)
    position = jnp.arange(seq_len, dtype=jnp.int32)
    group_width = PW // 4
    window_means = []
    for group_id, window in enumerate(pool_windows):
        lower_end = jnp.clip(position - window // 2, 0, seq_len)
        upper_end = jnp.clip(position - window // 2 + window, 0, seq_len)
        counts = (upper_end - lower_end).astype(jnp.float32)[:, None]
        columns = prefix[:, group_id * group_width:(group_id + 1) * group_width]
        window_means.append((columns[upper_end] - columns[lower_end]) / counts)
    pooled = ((jnp.concatenate(window_means, axis=1) - values) * pool_scale).astype(jnp.bfloat16)
    mixer_output = jnp.dot(pooled, w_mix_out, preferred_element_type=jnp.float32).astype(jnp.bfloat16)
    normed_expert = layer_norm(expert_rows, expert_gain)
    flat_route = routes.reshape(-1).astype(jnp.int32)
    onehot = (flat_route[:, None] == jnp.arange(EXPERTS, dtype=jnp.int32)[None, :]).astype(jnp.int32)
    running = jnp.cumsum(onehot.reshape(N_EP, TOK_DEV * TOP, EXPERTS), axis=1).reshape(-1, EXPERTS)
    ranking = lax.optimization_barrier(jnp.sum(onehot * (running - 1), axis=1))
    source_dev = jnp.arange(TOKENS * TOP, dtype=jnp.int32) // (TOK_DEV * TOP)
    slot_index = (flat_route * N_EP + source_dev) * CAP + ranking
    token_index = jnp.arange(TOKENS * TOP, dtype=jnp.int32) // TOP
    slot_table = jnp.zeros((EXPERTS * N_EP * CAP, D), jnp.bfloat16).at[slot_index].set(normed_expert[token_index])

    def run_expert(packed):
        slot_rows, gate_weight, up_weight, down_weight = packed
        gate_val = jnp.dot(slot_rows, gate_weight, preferred_element_type=jnp.float32)
        up_val = jnp.dot(slot_rows, up_weight, preferred_element_type=jnp.float32)
        hidden = (jax.nn.silu(gate_val) * up_val).astype(jnp.bfloat16)
        return jnp.dot(hidden, down_weight, preferred_element_type=jnp.float32).astype(jnp.bfloat16)
    results = lax.map(run_expert, (slot_table.reshape(EXPERTS, N_EP * CAP, D), expert_gate, expert_up, expert_down))
    picked = results.reshape(-1, D)[slot_index].astype(jnp.float32).reshape(TOKENS, TOP, D)
    expert_output = lax.optimization_barrier(jnp.sum(picked * route_weight[:, :, None], axis=1)).astype(jnp.bfloat16)
    return (mixer_output, expert_output)
```

```python
import jax
import jax.numpy as jnp
from jax import lax
from jax.sharding import PartitionSpec as P

PW = 2048
TOP = 2


norm_eps = 1e-05
pool_windows = (2, 4, 8, 16)
rim_rows = 8
group_count = 4


def swapped(block, axis, bits):
    count = lax.axis_size(axis)
    return lax.ppermute(block, axis, [(i, i ^ bits) for i in range(count)])


def gathered(block):
    if lax.axis_size("tp") != 4:
        return lax.all_gather(block, "tp", axis=1, tiled=True)
    half = block.shape[0] // 2
    first = swapped(block, "tp", 1)
    second = swapped(block, "tp", 2)
    top = swapped(first[:half], "tp", 2)
    bottom = swapped(second[half:], "tp", 1)
    return jnp.concatenate([block, first, second, jnp.concatenate([top, bottom], axis=0)], axis=1)


def arranged(weight, tp_index):
    count = lax.axis_size("tp")
    if count != 4:
        return weight
    width = weight.shape[0] // count
    return jnp.concatenate(
        [lax.dynamic_slice_in_dim(weight, (tp_index ^ j) * width, width, 0) for j in range(count)], axis=0
    )


def dot(a, b):
    return lax.dot_general(a, b, (((1,), (0,)), ((), ())), preferred_element_type=jnp.float32)


def row_stats(values):
    mean = jnp.mean(values, axis=1)
    center = values - mean[:, None]
    return mean, jnp.sum(center * center, axis=1)


def merged_stats(means, squares, width):
    mean = jnp.mean(means, axis=0)
    apart = means - mean[None, :]
    total = jnp.sum(squares, axis=0) + width * jnp.sum(apart * apart, axis=0)
    return mean, total / (width * means.shape[0])


def normed(values, mean, spread, gain):
    center = values - mean[:, None]
    return (center * lax.rsqrt(spread + norm_eps)[:, None] * gain[None, :]).astype(jnp.bfloat16)


def pooled_channels(inner, scale_local, ep_size, ep_index, tp_index):
    row_count, channels = inner.shape
    forward = [(i, i + 1) for i in range(ep_size - 1)]
    backward = [(target, source) for source, target in forward]
    low = lax.ppermute(inner[row_count - rim_rows :], "ep", forward)
    high = lax.ppermute(inner[:rim_rows], "ep", backward)
    extended = jnp.concatenate([low, inner, high], axis=0)
    group = tp_index * channels // (PW // len(pool_windows))
    window = jnp.left_shift(jnp.int32(pool_windows[0]), group)
    half_span = window // 2
    seq_len = row_count * ep_size
    row = jnp.arange(row_count, dtype=jnp.int32)[:, None]
    column = jnp.arange(row_count + 2 * rim_rows, dtype=jnp.int32)[None, :] - rim_rows
    band = ((column >= row - half_span) & (column < row + half_span)).astype(jnp.bfloat16)
    position = ep_index * row_count + row
    lower_end = jnp.clip(position - half_span, 0, seq_len)
    upper_end = jnp.clip(position - half_span + window, 0, seq_len)
    counts = (upper_end - lower_end).astype(jnp.float32)
    values = inner.astype(jnp.float32)
    return ((dot(band, extended) / counts - values) * scale_local[None, :]).astype(jnp.bfloat16)


def on_device(
    mixer_rows,
    expert_rows,
    mixer_gain,
    pool_scale,
    w_in,
    w_mix_out,
    expert_gain,
    expert_gate,
    expert_up,
    expert_down,
    routes,
    route_weight,
):
    ep_size = lax.axis_size("ep")
    tp_size = lax.axis_size("tp")
    ep_index = lax.axis_index("ep")
    tp_index = lax.axis_index("tp")
    row_count = routes.shape[0]
    width = expert_rows.shape[1]
    capacity = (3 * TOP * row_count + 2 * ep_size - 1) // (2 * ep_size)

    mix_values = mixer_rows.astype(jnp.float32)
    expert_values = expert_rows.astype(jnp.float32)
    own_stats = jnp.stack([*row_stats(mix_values), *row_stats(expert_values)])
    if tp_size == 4:
        stats = jnp.stack([own_stats] + [swapped(own_stats, "tp", j) for j in range(1, tp_size)])
    else:
        stats = lax.all_gather(own_stats, "tp", axis=0)
    mix_gain = lax.dynamic_slice_in_dim(mixer_gain, tp_index * width, width)
    rows_gain = lax.dynamic_slice_in_dim(expert_gain, tp_index * width, width)
    mix_normed = normed(mix_values, *merged_stats(stats[:, 0], stats[:, 1], width), mix_gain)
    rows_normed = normed(expert_values, *merged_stats(stats[:, 2], stats[:, 3], width), rows_gain)

    experts = jnp.arange(ep_size, dtype=jnp.int32)
    chosen = routes[:, :, None] == experts[None, None, :]
    named = (chosen[:, 0] | chosen[:, 1]).astype(jnp.bfloat16)
    row = jnp.arange(row_count, dtype=jnp.int32)
    earlier = (row[None, :] < row[:, None]).astype(jnp.bfloat16)
    ahead = dot(earlier, named)
    ranking = jnp.sum(jnp.where(chosen, ahead[:, None, :], 0.0), axis=2).astype(jnp.int32)
    place = (routes ^ ep_index) * capacity + ranking

    blocks = max(1, ep_size // group_count)
    span = blocks * capacity
    slot = jnp.arange(span, dtype=jnp.int32)

    full_mix = gathered(mix_normed)
    gate_up = arranged(jnp.concatenate([expert_gate[0], expert_up[0]], axis=1), tp_index)
    down_weight = arranged(expert_down[0], tp_index)
    inner = dot(full_mix, arranged(w_in, tp_index)).astype(jnp.bfloat16)
    pooled = pooled_channels(inner, pool_scale, ep_size, ep_index, tp_index)

    place_rows = place.T
    arrivals = []
    for start in range(0, ep_size, blocks):
        slots = slot + start * capacity
        picks = (slots[:, None] == place_rows[0][None, :]) | (slots[:, None] == place_rows[1][None, :])
        outgoing = dot(picks.astype(jnp.bfloat16), rows_normed).astype(jnp.bfloat16)
        pieces = []
        for b in range(blocks):
            piece = outgoing[b * capacity : (b + 1) * capacity]
            pieces.append(piece if start + b == 0 else swapped(piece, "ep", start + b))
        arrivals.append(jnp.concatenate(pieces, axis=0))

    hiddens = []
    for arrived in arrivals:
        both = dot(gathered(arrived), gate_up)
        units = both.shape[1] // 2
        hiddens.append((jax.nn.silu(both[:, :units]) * both[:, units:]).astype(jnp.bfloat16))

    total = jnp.zeros((row_count, expert_down.shape[2]), jnp.float32)
    for index, hidden in enumerate(hiddens):
        start = index * blocks
        value = dot(gathered(hidden), down_weight).astype(jnp.bfloat16)
        pieces = []
        for b in range(blocks):
            piece = value[b * capacity : (b + 1) * capacity]
            pieces.append(piece if start + b == 0 else swapped(piece, "ep", start + b))
        returned = jnp.concatenate(pieces, axis=0)
        slots = slot + start * capacity
        for k in range(TOP):
            picks = (place[:, k][:, None] == slots[None, :]).astype(jnp.bfloat16)
            total = total + dot(picks, returned) * route_weight[:, k][:, None]
    expert_output = total.astype(jnp.bfloat16)
    mixer_output = dot(gathered(pooled), arranged(w_mix_out, tp_index)).astype(jnp.bfloat16)
    return (mixer_output, expert_output)


def solution(mesh):
    return jax.shard_map(
        on_device,
        mesh=mesh,
        in_specs=(
            P("ep", "tp"),
            P("ep", "tp"),
            P(),
            P("tp"),
            P(None, "tp"),
            P(None, "tp"),
            P(),
            P("ep", None, "tp"),
            P("ep", None, "tp"),
            P("ep", None, "tp"),
            P("ep", None),
            P("ep", None),
        ),
        out_specs=(P("ep", "tp"), P("ep", "tp")),
        check_vma=False,
    )
```

```python
import jax
import jax.numpy as jnp
from jax import lax
from jax.sharding import PartitionSpec as P

PW = 2048
TOP = 2


norm_eps = 1e-05
pool_windows = (2, 4, 8, 16)
rim_rows = 8
group_count = 4


def swapped(block, axis, bits):
    count = lax.axis_size(axis)
    return lax.ppermute(block, axis, [(i, i ^ bits) for i in range(count)])


class Plane:
    def __init__(self):
        self.past = []

    def exchange(self, to_second, to_first):
        if len(self.past) > 1:
            to_second, to_first, *_ = lax.optimization_barrier((to_second, to_first, *self.past[-2]))
        result = (swapped(to_second, "tp", 2), swapped(to_first, "tp", 1))
        self.past.append(result)
        return result

    def begin(self, block):
        if lax.axis_size("tp") != 4:
            return block
        second, first = self.exchange(block, block)
        return block, first, second

    def finish(self, begun):
        if lax.axis_size("tp") != 4:
            return lax.all_gather(begun, "tp", axis=1, tiled=True)
        block, first, second = begun
        half = block.shape[0] // 2
        top, bottom = self.exchange(first[:half], second[half:])
        return jnp.concatenate([block, first, second, jnp.concatenate([top, bottom], axis=0)], axis=1)


def arranged(weight, tp_index):
    count = lax.axis_size("tp")
    if count != 4:
        return weight
    width = weight.shape[0] // count
    return jnp.concatenate(
        [lax.dynamic_slice_in_dim(weight, (tp_index ^ j) * width, width, 0) for j in range(count)], axis=0
    )


def dot(a, b):
    return lax.dot_general(a, b, (((1,), (0,)), ((), ())), preferred_element_type=jnp.float32)


def layer_norm(row_block, gain_vec):
    values = row_block.astype(jnp.float32)
    center = values - jnp.mean(values, axis=-1, keepdims=True)
    spread = jnp.mean(center * center, axis=-1, keepdims=True)
    return (center * lax.rsqrt(spread + norm_eps) * gain_vec).astype(jnp.bfloat16)


def pooled_channels(inner, scale_local, ep_size, ep_index, tp_index):
    row_count, channels = inner.shape
    forward = [(i, i + 1) for i in range(ep_size - 1)]
    backward = [(target, source) for source, target in forward]
    low = lax.ppermute(inner[row_count - rim_rows :], "ep", forward)
    high = lax.ppermute(inner[:rim_rows], "ep", backward)
    extended = jnp.concatenate([low, inner, high], axis=0)
    group = tp_index * channels // (PW // len(pool_windows))
    window = jnp.left_shift(jnp.int32(pool_windows[0]), group)
    half_span = window // 2
    seq_len = row_count * ep_size
    row = jnp.arange(row_count, dtype=jnp.int32)[:, None]
    column = jnp.arange(row_count + 2 * rim_rows, dtype=jnp.int32)[None, :] - rim_rows
    band = ((column >= row - half_span) & (column < row + half_span)).astype(jnp.bfloat16)
    position = ep_index * row_count + row
    lower_end = jnp.clip(position - half_span, 0, seq_len)
    upper_end = jnp.clip(position - half_span + window, 0, seq_len)
    counts = (upper_end - lower_end).astype(jnp.float32)
    values = inner.astype(jnp.float32)
    return ((dot(band, extended) / counts - values) * scale_local[None, :]).astype(jnp.bfloat16)


def on_device(
    mixer_rows,
    expert_rows,
    mixer_gain,
    pool_scale,
    w_in,
    w_mix_out,
    expert_gain,
    expert_gate,
    expert_up,
    expert_down,
    routes,
    route_weight,
):
    ep_size = lax.axis_size("ep")
    ep_index = lax.axis_index("ep")
    tp_index = lax.axis_index("tp")
    row_count = routes.shape[0]
    capacity = (3 * TOP * row_count + 2 * ep_size - 1) // (2 * ep_size)
    blocks = max(1, ep_size // group_count)
    groups = ep_size // blocks
    slot = jnp.arange(blocks * capacity, dtype=jnp.int32)
    plane = Plane()

    mix = plane.begin(mixer_rows)

    experts = jnp.arange(ep_size, dtype=jnp.int32)
    chosen = routes[:, :, None] == experts[None, None, :]
    named = (chosen[:, 0] | chosen[:, 1]).astype(jnp.bfloat16)
    row = jnp.arange(row_count, dtype=jnp.int32)
    earlier = (row[None, :] < row[:, None]).astype(jnp.bfloat16)
    ahead = dot(earlier, named)
    ranking = jnp.sum(jnp.where(chosen, ahead[:, None, :], 0.0), axis=2).astype(jnp.int32)
    place = (routes ^ ep_index) * capacity + ranking
    place_rows = place.T

    def crossed(rows, group):
        pieces = []
        for b in range(blocks):
            shift = group * blocks + b
            piece = rows[b * capacity : (b + 1) * capacity]
            pieces.append(piece if shift == 0 else swapped(piece, "ep", shift))
        return jnp.concatenate(pieces, axis=0)

    order = [0] + list(range(groups - 1, 0, -1))
    arrived = {}
    after = place_rows
    for group in order:
        slots = slot + group * blocks * capacity
        picks = (slots[:, None] == after[0][None, :]) | (slots[:, None] == after[1][None, :])
        outgoing = dot(picks.astype(jnp.bfloat16), expert_rows).astype(jnp.bfloat16)
        after, outgoing = lax.optimization_barrier((place_rows, outgoing))
        arrived[group] = crossed(outgoing, group)

    gain = arranged(expert_gain, tp_index)
    gate_up = arranged(jnp.concatenate([expert_gate[0], expert_up[0]], axis=1), tp_index)
    down_weight = arranged(expert_down[0], tp_index)

    def hidden_of(slots):
        both = dot(layer_norm(slots, gain), gate_up)
        units = both.shape[1] // 2
        return (jax.nn.silu(both[:, :units]) * both[:, units:]).astype(jnp.bfloat16)

    returned = {}

    def send_back(group, begun):
        full = plane.finish(begun)
        value = dot(full, down_weight).astype(jnp.bfloat16)
        returned[group] = crossed(value, group)

    hidden = {}
    rows = plane.begin(arrived[0])
    full_mix = plane.finish(mix)
    hidden[0] = hidden_of(plane.finish(rows))
    mix_weight = arranged(w_in, tp_index)
    mix_normed = layer_norm(full_mix, arranged(mixer_gain, tp_index))
    inner = dot(mix_normed, mix_weight).astype(jnp.bfloat16)
    pooled = pooled_channels(inner, pool_scale, ep_size, ep_index, tp_index)
    waiting = plane.begin(pooled)
    finish_mix = True
    behind = None
    for group in order[1:]:
        rows = plane.begin(arrived[group])
        if finish_mix:
            full_pooled = plane.finish(waiting)
            out_weight = arranged(w_mix_out, tp_index)
            mixer_output = dot(full_pooled, out_weight).astype(jnp.bfloat16)
            finish_mix = False
        else:
            hidden[behind[0]] = hidden_of(plane.finish(behind[1]))
        behind = (group, rows)
    queue = order[1:] + order[:1]
    begun = plane.begin(hidden[queue[0]])
    hidden[behind[0]] = hidden_of(plane.finish(behind[1]))
    for index, group in enumerate(queue):
        if index + 1 < len(queue):
            following = plane.begin(hidden[queue[index + 1]])
        send_back(group, begun)
        begun = following

    total = jnp.zeros((row_count, expert_down.shape[2]), jnp.float32)
    for group in queue:
        slots = slot + group * blocks * capacity
        for k in range(TOP):
            picks = (place[:, k][:, None] == slots[None, :]).astype(jnp.bfloat16)
            total = total + dot(picks, returned[group]) * route_weight[:, k][:, None]
    return (mixer_output, total.astype(jnp.bfloat16))


def solution(mesh):
    return mapped(mesh)


def mapped(mesh):
    return jax.shard_map(
        on_device,
        mesh=mesh,
        in_specs=(
            P("ep", "tp"),
            P("ep", "tp"),
            P(),
            P("tp"),
            P(None, "tp"),
            P(None, "tp"),
            P(),
            P("ep", None, "tp"),
            P("ep", None, "tp"),
            P("ep", None, "tp"),
            P("ep", None),
            P("ep", None),
        ),
        out_specs=(P("ep", "tp"), P("ep", "tp")),
        check_vma=False,
    )
```

```python
import jax
import jax.numpy as jnp
from jax import lax
from jax.sharding import PartitionSpec as P

PW = 2048
TOP = 2


norm_eps = 1e-05
pool_windows = (2, 4, 8, 16)
rim_rows = 8
group_count = 4


def swapped(block, axis, bits):
    count = lax.axis_size(axis)
    return lax.ppermute(block, axis, [(i, i ^ bits) for i in range(count)])


class Plane:
    def __init__(self):
        self.past = []

    def exchange(self, to_second, to_first):
        if len(self.past) > 2:
            to_second, to_first, *_ = lax.optimization_barrier((to_second, to_first, *self.past[-3]))
        result = (swapped(to_second, "tp", 2), swapped(to_first, "tp", 1))
        self.past.append(result)
        return result

    def begin(self, block):
        if lax.axis_size("tp") != 4:
            return block
        second, first = self.exchange(block, block)
        return block, first, second

    def finish(self, begun):
        if lax.axis_size("tp") != 4:
            return lax.all_gather(begun, "tp", axis=1, tiled=True)
        block, first, second = begun
        half = block.shape[0] // 2
        upper, lower = first[:half], second[half:]
        top, bottom = self.exchange(upper, lower)
        return jnp.concatenate([block, first, second, jnp.concatenate([top, bottom], axis=0)], axis=1)


def arranged(weight, tp_index):
    count = lax.axis_size("tp")
    if count != 4:
        return weight
    width = weight.shape[0] // count
    return jnp.concatenate(
        [lax.dynamic_slice_in_dim(weight, (tp_index ^ j) * width, width, 0) for j in range(count)], axis=0
    )


def dot(a, b):
    return lax.dot_general(a, b, (((1,), (0,)), ((), ())), preferred_element_type=jnp.float32)


def layer_norm(row_block, gain_vec):
    values = row_block.astype(jnp.float32)
    center = values - jnp.mean(values, axis=-1, keepdims=True)
    spread = jnp.mean(center * center, axis=-1, keepdims=True)
    return (center * lax.rsqrt(spread + norm_eps) * gain_vec).astype(jnp.bfloat16)


def pooled_channels(inner, scale_local, ep_size, ep_index, tp_index):
    row_count, channels = inner.shape
    forward = [(i, i + 1) for i in range(ep_size - 1)]
    backward = [(target, source) for source, target in forward]
    low = lax.ppermute(inner[row_count - rim_rows :], "ep", forward)
    high = lax.ppermute(inner[:rim_rows], "ep", backward)
    extended = jnp.concatenate([low, inner, high], axis=0)
    group = tp_index * channels // (PW // len(pool_windows))
    window = jnp.left_shift(jnp.int32(pool_windows[0]), group)
    half_span = window // 2
    seq_len = row_count * ep_size
    row = jnp.arange(row_count, dtype=jnp.int32)[:, None]
    column = jnp.arange(row_count + 2 * rim_rows, dtype=jnp.int32)[None, :] - rim_rows
    band = ((column >= row - half_span) & (column < row + half_span)).astype(jnp.bfloat16)
    position = ep_index * row_count + row
    lower_end = jnp.clip(position - half_span, 0, seq_len)
    upper_end = jnp.clip(position - half_span + window, 0, seq_len)
    counts = (upper_end - lower_end).astype(jnp.float32)
    values = inner.astype(jnp.float32)
    return ((dot(band, extended) / counts - values) * scale_local[None, :]).astype(jnp.bfloat16)


def on_device(
    mixer_rows,
    expert_rows,
    mixer_gain,
    pool_scale,
    w_in,
    w_mix_out,
    expert_gain,
    expert_gate,
    expert_up,
    expert_down,
    routes,
    route_weight,
):
    ep_size = lax.axis_size("ep")
    ep_index = lax.axis_index("ep")
    tp_index = lax.axis_index("tp")
    row_count = routes.shape[0]
    capacity = (3 * TOP * row_count + 2 * ep_size - 1) // (2 * ep_size)
    blocks = max(1, ep_size // group_count)
    groups = ep_size // blocks
    slot = jnp.arange(blocks * capacity, dtype=jnp.int32)
    plane = Plane()

    mix = plane.begin(mixer_rows)

    experts = jnp.arange(ep_size, dtype=jnp.int32)
    chosen = routes[:, :, None] == experts[None, None, :]
    named = (chosen[:, 0] | chosen[:, 1]).astype(jnp.bfloat16)
    row = jnp.arange(row_count, dtype=jnp.int32)
    earlier = (row[None, :] < row[:, None]).astype(jnp.bfloat16)
    ahead = dot(earlier, named)
    ranking = jnp.sum(jnp.where(chosen, ahead[:, None, :], 0.0), axis=2).astype(jnp.int32)
    place = (routes ^ ep_index) * capacity + ranking
    place_rows = place.T

    def crossed(rows, group):
        pieces = []
        for b in range(blocks):
            shift = group * blocks + b
            piece = rows[b * capacity : (b + 1) * capacity]
            pieces.append(piece if shift == 0 else swapped(piece, "ep", shift))
        return jnp.concatenate(pieces, axis=0)

    order = [0] + list(range(groups - 1, 0, -1))
    arrived = {}
    after = place_rows
    for group in order:
        slots = slot + group * blocks * capacity
        picks = (slots[:, None] == after[0][None, :]) | (slots[:, None] == after[1][None, :])
        outgoing = dot(picks.astype(jnp.bfloat16), expert_rows).astype(jnp.bfloat16)
        after, outgoing = lax.optimization_barrier((place_rows, outgoing))
        arrived[group] = crossed(outgoing, group)

    gain = arranged(expert_gain, tp_index)
    gate_up = arranged(jnp.concatenate([expert_gate[0], expert_up[0]], axis=1), tp_index)
    down_weight = arranged(expert_down[0], tp_index)

    def hidden_of(slots):
        both = dot(layer_norm(slots, gain), gate_up)
        units = both.shape[1] // 2
        return (jax.nn.silu(both[:, :units]) * both[:, units:]).astype(jnp.bfloat16)

    returned = {}

    def send_back(group, begun):
        full = plane.finish(begun)
        value = dot(full, down_weight).astype(jnp.bfloat16)
        returned[group] = crossed(value, group)

    hidden = {}
    rows = plane.begin(arrived[0])
    full_mix = plane.finish(mix)
    hidden[0] = hidden_of(plane.finish(rows))
    mix_weight = arranged(w_in, tp_index)
    mix_normed = layer_norm(full_mix, arranged(mixer_gain, tp_index))
    inner = dot(mix_normed, mix_weight).astype(jnp.bfloat16)
    pooled = pooled_channels(inner, pool_scale, ep_size, ep_index, tp_index)
    waiting = plane.begin(pooled)
    finish_mix = True
    behind = None
    for group in order[1:]:
        rows = plane.begin(arrived[group])
        if finish_mix:
            full_pooled = plane.finish(waiting)
            out_weight = arranged(w_mix_out, tp_index)
            mixer_output = dot(full_pooled, out_weight).astype(jnp.bfloat16)
            finish_mix = False
        else:
            hidden[behind[0]] = hidden_of(plane.finish(behind[1]))
        behind = (group, rows)
    queue = order[1:] + order[:1]
    begun = plane.begin(hidden[queue[0]])
    hidden[behind[0]] = hidden_of(plane.finish(behind[1]))
    for index, group in enumerate(queue):
        if index + 1 < len(queue):
            following = plane.begin(hidden[queue[index + 1]])
        send_back(group, begun)
        begun = following

    total = jnp.zeros((row_count, expert_down.shape[2]), jnp.float32)
    for group in queue:
        slots = slot + group * blocks * capacity
        for k in range(TOP):
            picks = (place[:, k][:, None] == slots[None, :]).astype(jnp.bfloat16)
            total = total + dot(picks, returned[group]) * route_weight[:, k][:, None]
    return (mixer_output, total.astype(jnp.bfloat16))


def solution(mesh):
    return mapped(mesh)


def mapped(mesh):
    return jax.shard_map(
        on_device,
        mesh=mesh,
        in_specs=(
            P("ep", "tp"),
            P("ep", "tp"),
            P(),
            P("tp"),
            P(None, "tp"),
            P(None, "tp"),
            P(),
            P("ep", None, "tp"),
            P("ep", None, "tp"),
            P("ep", None, "tp"),
            P("ep", None),
            P("ep", None),
        ),
        out_specs=(P("ep", "tp"), P("ep", "tp")),
        check_vma=False,
    )
```
